128 devices in a mesh: sp: 32 (over z, y, core), tp: 4 (over x).
Axes of the slice: x: 4, y: 4, z: 4, core: 2. Of those that a mesh axis runs over, the one named last changes fastest.
Arguments:
- tokens: bfloat16 [32768, 2048], P('sp', 'tp'), may hold values from -6 to 6
- input_norm_gain: float32 [2048], replicated, may hold values from 0.1 to 1.9
- pooling_input_matrix: bfloat16 [2048, 512], P(None, 'tp'), may hold values from -0.125 to 0.125
- query_projection_matrix: bfloat16 [2048, 1024], P(None, 'tp'), may hold values from -0.125 to 0.125
- key_projection_matrix: bfloat16 [2048, 1024], P(None, 'tp'), may hold values from -0.125 to 0.125
- value_projection_matrix: bfloat16 [2048, 1024], P(None, 'tp'), may hold values from -0.125 to 0.125
- output_gate_matrix: bfloat16 [2048, 1024], P(None, 'tp'), may hold values from -0.125 to 0.125
- input_gate_matrix: bfloat16 [2048, 2, 8], replicated
- forget_gate_matrix: bfloat16 [2048, 2, 8], replicated, may hold values from -0.125 to 0.125
- forget_gate_bias: float32 [2, 8], replicated
- log_forget_scale: float32 [2, 32768], P(None, 'sp'), may hold values from 0.35 to 2.8
- extra_log_forget: float32 [2, 32768], P(None, 'sp'), may hold values from -0.7 to 0, as said below
- starting_memory: float32 [2, 8, 128, 128], P(None, 'tp'), may hold values from -3 to 3
- starting_normalizer: float32 [2, 8, 128], P(None, 'tp'), may hold values from -3 to 3
- starting_log_scale: float32 [2, 8], P(None, 'tp'), may hold values from 2 to 5
- pooling_group_map: bfloat16 [4, 128, 128], replicated, may hold values from -0.5 to 0.5
- pooling_channel_scale: float32 [512], replicated, may hold values from 0.1 to 1.9
- memory_head_gain: float32 [1024], replicated, may hold values from 0.1 to 1.9
- pooling_output_matrix: bfloat16 [512, 2048], replicated, may hold values from -0.25 to 0.25
- memory_output_matrix: bfloat16 [1024, 2048], replicated, may hold values from -0.1875 to 0.1875
Outputs:
- mixed_out: bfloat16 [32768, 2048], P(('sp', 'tp'))
The draws below stay inside these ranges and needn't reach their ends.
Inputs may be any that keep to these rules, and one draw needn't show every extreme that they name: `extra_log_forget`: at most three nonzero entries in each direction.
All inputs are finite; a program needn't handle non-finite values.
Results may differ from the reference program's by a relative error of at most 0.0091.
Values may be sent and summed in bfloat16 or wider, within the bound.
A program may use at most 128 MiB of HBM per device.

```python
import jax
import jax.numpy as jnp
from jax import lax

D = 2048
POOL_GROUPS = 4
GROUP_DIM = 128
HEADS = 8
DH = 128
BLOCK = 128
TOK_DEV = 1024
POOL_W = 512
MEM_W = 1024
TOKENS = 32768


def draw_forget_gate_bias(key, part):
    pick_key, slow_key, fast_key = jax.random.split(key, 3)
    slow_share = 0.5
    slow_heads = jax.random.uniform(pick_key, (2, HEADS)) < slow_share
    slow_bias = jnp.log(jnp.float32(TOKENS)) + jax.random.uniform(slow_key, (2, HEADS), minval=1.5, maxval=2.5)
    fast_bias = jax.random.uniform(fast_key, (2, HEADS), minval=3.8, maxval=4.8)
    return jnp.where(slow_heads, slow_bias, fast_bias).astype(jnp.float32)


def draw_log_forget_scale(key, part):
    block_key, rough_key = jax.random.split(key)
    segments = TOKENS // TOK_DEV
    block_factor = jnp.exp(jax.random.uniform(block_key, (2, segments, 1), minval=-0.69, maxval=0.69))
    rough_factor = jax.random.uniform(rough_key, (2, segments, TOK_DEV), minval=0.7, maxval=1.4)
    return (block_factor * rough_factor).reshape(2, TOKENS).astype(jnp.float32)


def draw_extra_log_forget(key, part):
    first_key, second_key, depth_key = jax.random.split(key, 3)
    first_places = jax.random.permutation(first_key, TOKENS)[:3]
    second_places = jax.random.permutation(second_key, TOKENS)[:3]
    places = jnp.stack([first_places, second_places]).astype(jnp.int32)
    depths = jnp.log(jax.random.uniform(depth_key, (2, 3), minval=0.5, maxval=0.8))
    direction_rows = jnp.arange(2)[:, None]
    return jnp.zeros((2, TOKENS), jnp.float32).at[direction_rows, places].set(depths)


def draw_input_gate_matrix(key, part):
    base_key = jax.random.fold_in(key, 0)
    weights = jax.random.normal(base_key, (D, 2, HEADS), jnp.float32) * D ** (-0.5)
    return weights.astype(jnp.bfloat16)


def block_levels(own_key, extent, cuts, smallest, top_value):
    def one(dim, parts):
        steps = jax.random.uniform(jax.random.fold_in(jax.random.fold_in(own_key, 6), dim), (parts,), jnp.float32, smallest / len(cuts), top_value / len(cuts))
        return jnp.repeat(jnp.exp(steps), extent[dim] // parts).reshape((-1,) + (1,) * (len(extent) - dim - 1))

    factor_of = one(*cuts[0])
    for cut in cuts[1:]:
        factor_of = factor_of * one(*cut)
    return factor_of


def gaussian(own_key, dims, deviation, bound, cuts=(), kind=jnp.bfloat16):
    array = jax.random.normal(own_key, dims, jnp.float32) * deviation
    if len(cuts) > 0:
        array = block_levels(own_key, dims, cuts, -0.22, 0.18) * array
    return jnp.clip(array, min=-bound, max=bound).astype(kind)


def setup_inputs(seed: int = 0) -> dict:
    keys = jax.random.split(jax.random.key(seed), 21)
    return {
        "tokens": gaussian(keys[0], (TOKENS, D), 1.0, 6.0, ((0, 32), (1, 4))),
        "input_norm_gain": jnp.clip(1.0 + 0.18 * jax.random.normal(keys[1], (D,), jnp.float32), 0.1, 1.9),
        "pooling_input_matrix": gaussian(keys[2], (D, POOL_W), D ** -0.5, 0.125, ((1, 4),)),
        "query_projection_matrix": gaussian(keys[3], (D, MEM_W), D ** -0.5, 0.125, ((1, 4),)),
        "key_projection_matrix": gaussian(keys[4], (D, MEM_W), D ** -0.5, 0.125, ((1, 4),)),
        "value_projection_matrix": gaussian(keys[5], (D, MEM_W), D ** -0.5, 0.125, ((1, 4),)),
        "output_gate_matrix": gaussian(keys[6], (D, MEM_W), D ** -0.5, 0.125, ((1, 4),)),
        "input_gate_matrix": draw_input_gate_matrix(jax.random.fold_in(keys[20], 71), 0),
        "forget_gate_matrix": gaussian(keys[8], (D, 2, HEADS), D ** -0.5, 0.125),
        "forget_gate_bias": draw_forget_gate_bias(jax.random.fold_in(keys[20], 71), 0),
        "log_forget_scale": draw_log_forget_scale(jax.random.fold_in(keys[20], 71), 0),
        "extra_log_forget": draw_extra_log_forget(jax.random.fold_in(keys[20], 71), 0),
        "starting_memory": gaussian(keys[12], (2, HEADS, DH, DH), 0.5, 3.0, ((1, 4),), jnp.float32),
        "starting_normalizer": gaussian(keys[13], (2, HEADS, DH), 0.5, 3.0, ((1, 4),), jnp.float32),
        "starting_log_scale": jnp.clip(2.0 + 3.0 * jax.random.uniform(keys[14], (2, HEADS), jnp.float32) ** block_levels(keys[14], (2, HEADS), ((1, 4),), -0.2, 0.2), 2.0, 5.0),
        "pooling_group_map": gaussian(keys[15], (POOL_GROUPS, GROUP_DIM, GROUP_DIM), GROUP_DIM ** -0.5, 0.5),
        "pooling_channel_scale": jnp.clip(1.0 + 0.18 * jax.random.normal(keys[16], (POOL_W,), jnp.float32), 0.1, 1.9),
        "memory_head_gain": jnp.clip(1.0 + 0.18 * jax.random.normal(keys[17], (MEM_W,), jnp.float32), 0.1, 1.9),
        "pooling_output_matrix": gaussian(keys[18], (POOL_W, D), POOL_W ** -0.5, 0.25),
        "memory_output_matrix": gaussian(keys[19], (MEM_W, D), MEM_W ** -0.5, 0.1875),
    }


NEG_BIG = -1e+30
LN_EPS = 1e-05
HEAD_EPS = 1e-06
HIGHEST = lax.Precision.HIGHEST

def block_step(carried, pieces):
    memory, normer, maxlog = carried
    q_blk, k_blk, v_blk, i_blk, f_blk = pieces
    lower_mask = jnp.tril(jnp.ones((BLOCK, BLOCK), dtype=bool))
    cumulative = jnp.cumsum(f_blk, axis=-1)
    exponent = jnp.where(lower_mask, cumulative[:, :, None] - cumulative[:, None, :] + i_blk[:, None, :], NEG_BIG)
    carried_log = cumulative + maxlog[:, None]
    row_max = jnp.maximum(carried_log, exponent.max(-1))
    fading = jnp.exp(carried_log - row_max)
    scores = jnp.einsum('htd,hsd->hts', q_blk, k_blk, precision=HIGHEST) * jnp.exp(exponent - row_max[:, :, None])
    numerator = fading[:, :, None] * jnp.einsum('hvk,htk->htv', memory, q_blk, precision=HIGHEST) + jnp.einsum('hts,hsv->htv', scores, v_blk, precision=HIGHEST)
    denominator = fading * jnp.einsum('hk,htk->ht', normer, q_blk, precision=HIGHEST) + scores.sum(-1)
    summed = cumulative[:, -1]
    weight_log = summed[:, None] - cumulative + i_blk
    new_max = jnp.maximum(summed + maxlog, weight_log.max(-1))
    carry_scale = jnp.exp(summed + maxlog - new_max)
    weights = jnp.exp(weight_log - new_max[:, None])
    memory = carry_scale[:, None, None] * memory + jnp.einsum('hsv,hsk->hvk', v_blk * weights[:, :, None], k_blk, precision=HIGHEST)
    normer = carry_scale[:, None] * normer + jnp.einsum('hs,hsk->hk', weights, k_blk, precision=HIGHEST)
    return ((memory, normer, new_max), (numerator, denominator, row_max))

def to_blocks(source):
    return jnp.moveaxis(source.reshape((source.shape[0], source.shape[1] // BLOCK, BLOCK) + source.shape[2:]), 1, 0)

def from_blocks(source):
    return jnp.moveaxis(source, 0, 1).reshape((source.shape[1], source.shape[0] * source.shape[2]) + source.shape[3:])

def memory_direction(query_heads, key_heads, value_heads, log_in, log_forget_gate, initial):
    finals, outputs = lax.scan(block_step, initial, tuple((to_blocks(member) for member in (query_heads, key_heads, value_heads, log_in, log_forget_gate))))
    numerator, denominator, row_max = (from_blocks(member) for member in outputs)
    return numerator / jnp.maximum(jnp.abs(denominator), 1.0)[:, :, None]

def reference(tokens, input_norm_gain, pooling_input_matrix, query_projection_matrix, key_projection_matrix, value_projection_matrix, output_gate_matrix, input_gate_matrix, forget_gate_matrix, forget_gate_bias, log_forget_scale, extra_log_forget, starting_memory, starting_normalizer, starting_log_scale, pooling_group_map, pooling_channel_scale, memory_head_gain, pooling_output_matrix, memory_output_matrix):
    total_rows = tokens.shape[0]
    model_width = tokens.shape[1]
    floats = tokens.astype(jnp.float32)
    mean_row = lax.optimization_barrier(jnp.sum(floats, axis=1)) / model_width
    square_mean = lax.optimization_barrier(jnp.sum(floats * floats, axis=1)) / model_width
    variance = square_mean - mean_row * mean_row
    normed = ((floats - mean_row[:, None]) * lax.rsqrt(variance + LN_EPS)[:, None] * input_norm_gain).astype(jnp.bfloat16)

    def project(weight):
        return jnp.dot(normed, weight, preferred_element_type=jnp.float32)
    pool_in = project(pooling_input_matrix).astype(jnp.bfloat16)
    queries = project(query_projection_matrix).astype(jnp.bfloat16)
    key_rows = project(key_projection_matrix).astype(jnp.bfloat16)
    value_rows = project(value_projection_matrix).astype(jnp.bfloat16)
    out_gate = project(output_gate_matrix).astype(jnp.bfloat16)
    in_pre = project(input_gate_matrix.reshape(model_width, 2 * HEADS)).reshape(total_rows, 2, HEADS)
    forget_gate_preact = project(forget_gate_matrix.reshape(model_width, 2 * HEADS)).reshape(total_rows, 2, HEADS)
    log_forget_gate = jax.nn.log_sigmoid(forget_gate_preact + forget_gate_bias[None]) * log_forget_scale.T[:, :, None] + extra_log_forget.T[:, :, None]

    def heads_of(source, factor):
        return (source.astype(jnp.float32) * factor).reshape(total_rows, HEADS, DH).transpose(1, 0, 2)
    query_heads = heads_of(queries, 1.0)
    key_heads = heads_of(key_rows, DH ** (-0.5))
    value_heads = heads_of(value_rows, 1.0)
    forward = memory_direction(query_heads, key_heads, value_heads, in_pre[:, 0].T, log_forget_gate[:, 0].T, (starting_memory[0], starting_normalizer[0], starting_log_scale[0]))
    backward = memory_direction(query_heads[:, ::-1], key_heads[:, ::-1], value_heads[:, ::-1], in_pre[:, 1].T[:, ::-1], log_forget_gate[:, 1].T[:, ::-1], (starting_memory[1], starting_normalizer[1], starting_log_scale[1]))
    hidden = forward + backward[:, ::-1]
    head_mean = lax.optimization_barrier(jnp.mean(hidden, axis=-1, keepdims=True))
    head_var = lax.optimization_barrier(jnp.mean(jnp.square(hidden - head_mean), axis=-1, keepdims=True))
    scaled = (hidden - head_mean) * lax.rsqrt(head_var + HEAD_EPS) * memory_head_gain.reshape(HEADS, DH)[:, None, :]
    mem_out = (scaled.transpose(1, 0, 2).reshape(total_rows, HEADS * DH) * jax.nn.sigmoid(out_gate.astype(jnp.float32))).astype(jnp.bfloat16)
    positions = jnp.arange(total_rows, dtype=jnp.int32)
    group_outs = []
    for group_index in range(POOL_GROUPS):
        half_span = 2 ** group_index
        grouped = pool_in[:, group_index * GROUP_DIM:(group_index + 1) * GROUP_DIM].astype(jnp.float32)
        padded = jnp.pad(grouped, ((half_span, half_span), (0, 0)))
        pooled = jnp.zeros_like(grouped)
        for offset in range(-half_span, half_span):
            pooled = pooled + padded[half_span + offset:half_span + offset + total_rows]
        upper_edge = jnp.minimum(positions + half_span, total_rows)
        lower_edge = jnp.maximum(positions - half_span, 0)
        counts = (upper_edge - lower_edge).astype(jnp.float32)
        contrast = (pooled / counts[:, None] - grouped).astype(jnp.bfloat16)
        mapped = jnp.dot(contrast, pooling_group_map[group_index], preferred_element_type=jnp.float32)
        group_outs.append((mapped * pooling_channel_scale[group_index * GROUP_DIM:(group_index + 1) * GROUP_DIM]).astype(jnp.bfloat16))
    pool_out = jnp.concatenate(group_outs, axis=1)
    mixed = jnp.dot(pool_out, pooling_output_matrix, preferred_element_type=jnp.float32) + jnp.dot(mem_out, memory_output_matrix, preferred_element_type=jnp.float32)
    return mixed.astype(jnp.bfloat16)
```

```python
import functools
import math

import jax
import jax.numpy as jnp
from jax import lax
from jax.experimental import pallas as pl
from jax.experimental.pallas import tpu as pltpu
from jax.sharding import PartitionSpec as P

DH = 128
EXT = 144
TP = 4
MARGIN = 64
RIM = 16
NEG_BIG = -1e30
LN_EPS = 1e-05
HEAD_EPS = 1e-06
MESH = pl.DeviceIdType.MESH
F32 = jnp.float32
BF16 = jnp.bfloat16
TRANS_B = (((1,), (1,)), ((), ()))


def dot(a, b):
    return jnp.dot(a, b, preferred_element_type=F32)


def dot_t(a, b):
    return lax.dot_general(a, b, TRANS_B, preferred_element_type=F32)


def combine(items):
    after = None
    logs = []
    for fall, top in reversed(items):
        logs.append(top if after is None else top + after)
        after = fall if after is None else after + fall
    logs.reverse()
    joint = functools.reduce(jnp.maximum, logs)
    return [jnp.exp(one - joint) for one in logs], after, joint


def kernel(
    ny,
    nz,
    tok,
    gain,
    wp_hbm,
    wq_hbm,
    wk_hbm,
    wv_hbm,
    wo_hbm,
    gin,
    gfg,
    bias,
    fscale,
    fextra,
    start_c,
    start_n,
    start_m,
    gmap,
    pscale,
    hgain,
    wpo_hbm,
    wmo_hbm,
    out,
    xg,
    wp,
    wq,
    wk,
    wv,
    wo,
    wpo,
    wmo,
    nb,
    qs,
    ks,
    vt,
    og,
    pool,
    gt,
    gsc,
    tri,
    xl,
    ar,
    cst,
    bs,
    ms,
    sum_c,
    sum_s,
    r0_c,
    r0_s,
    y_c,
    y_s,
    z_c,
    z_s,
    p_c,
    p_s,
    r3_c,
    r3_s,
    ent_c,
    ent_m,
    est,
    em,
    psend,
    pbuf,
    msend,
    mbuf,
    acc,
    load_sem,
    own_ss,
    own_rs,
    fwd_ss,
    fwd_rs,
    r0_ss,
    r0_rs,
    y_ss,
    y_rs,
    z_ss,
    z_rs,
    r3_ss,
    r3_rs,
    halo_ss,
    halo_rs,
    pool_ss,
    pool_rs,
    mem_ss,
    mem_rs,
):
    rows = tok.shape[0]
    width = tok.shape[1]
    ch = rows // TP
    hf = ch // 2
    t = lax.axis_index("tp")
    s = lax.axis_index("sp")
    ns = 2 * ny * nz
    core = lax.rem(s, 2)
    yi = lax.rem(s // 2, ny)
    zi = s // (2 * ny)
    partner = s + 1 - 2 * core
    right = lax.rem(t + 1, TP)
    left = lax.rem(t + 3, TP)
    step = 1 - 2 * core
    half_log = F32(0) + (-0.5 * math.log(DH))

    loads = []
    for index, (src, dst) in enumerate(
        (
            (wq_hbm, wq),
            (wk_hbm, wk),
            (wv_hbm, wv),
            (wo_hbm, wo),
            (wp_hbm, wp),
            (wpo_hbm, wpo),
            (wmo_hbm, wmo),
            (tok, xg.at[t]),
        )
    ):
        loads.append(pltpu.make_async_copy(src, dst, load_sem.at[index]))
    loads[7].start()

    barrier = pltpu.get_barrier_semaphore()
    peers = [(s, lax.rem(t + j, TP)) for j in range(1, TP)]
    peers.append((partner, t))
    peers += [((zi * ny + lax.rem(yi + j, ny)) * 2 + core, t) for j in range(1, ny)]
    peers += [((lax.rem(zi + j, nz) * ny + yi) * 2 + core, t) for j in range(1, nz)]
    peers += [(lax.rem(s + 1, ns), t), (lax.rem(s + ns - 1, ns), t)]
    pool[0:MARGIN] = jnp.zeros((MARGIN, DH), BF16)
    pool[MARGIN + rows : 2 * MARGIN + rows] = jnp.zeros((MARGIN, DH), BF16)
    z_c[...] = jnp.zeros_like(z_c)
    z_s[...] = jnp.zeros_like(z_s)
    for peer in peers:
        pl.semaphore_signal(barrier, inc=1, device_id=peer, device_id_type=MESH)
    pl.semaphore_wait(barrier, len(peers))

    def own_copy(c, way):
        span = pl.ds(pl.multiple_of(c * ch, ch), ch)
        return pltpu.make_async_remote_copy(
            src_ref=tok.at[span],
            dst_ref=xg.at[t, span],
            send_sem=own_ss.at[way, c],
            recv_sem=own_rs.at[way, c],
            device_id=(s, right if way == 0 else left),
            device_id_type=MESH,
        )

    def fwd_copy(c, way):
        span = pl.ds(pl.multiple_of(c * ch + way * hf, hf), hf)
        slot = left if way == 0 else right
        return pltpu.make_async_remote_copy(
            src_ref=xg.at[slot, span],
            dst_ref=xg.at[slot, span],
            send_sem=fwd_ss.at[way, c],
            recv_sem=fwd_rs.at[way, c],
            device_id=(s, right if way == 0 else left),
            device_id_type=MESH,
        )

    for c in (0, 1):
        for way in (0, 1):
            own_copy(c, way).start()
    for one in loads[:7]:
        one.start()

    gt[...] = jnp.concatenate(
        [gin[0].astype(F32), gin[1].astype(F32), gfg[0].astype(F32), gfg[1].astype(F32)], axis=0
    ).astype(BF16)
    row_of = lax.broadcasted_iota(jnp.int32, (ch, ch), 0)
    col_of = lax.broadcasted_iota(jnp.int32, (ch, ch), 1)
    tri[:, 0:ch] = jnp.where(row_of <= col_of, 1.0, 0.0).astype(BF16)
    tri[:, ch : 2 * ch] = jnp.where(row_of >= col_of, 1.0, 0.0).astype(BF16)
    tail = lax.broadcasted_iota(jnp.int32, (EXT - DH, rows), 0)
    ones_row = jnp.where(tail == 0, 1.0, 0.0).astype(BF16)
    for h in range(2):
        vt[h, DH:EXT, :] = ones_row

    loads[7].wait()
    for way in (0, 1):
        own_copy(0, way).wait_recv()
        fwd_copy(0, way).start()
        own_copy(2, way).start()
    for one in loads[:5]:
        one.wait()

    def chunk(c, carry):
        @pl.when(c + 1 < TP)
        def _():
            for way in (0, 1):
                own_copy(c + 1, way).wait_recv()
                fwd_copy(c + 1, way).start()

        @pl.when(c + 3 < TP)
        def _():
            for way in (0, 1):
                own_copy(c + 3, way).start()

        for way in (0, 1):
            slot = left if way == 0 else right
            span = pl.ds(pl.multiple_of(c * ch + way * hf, hf), hf)
            far = lax.rem(t + 2, TP)
            pltpu.make_async_remote_copy(
                src_ref=xg.at[far, span],
                dst_ref=xg.at[far, span],
                send_sem=fwd_ss.at[way, c],
                recv_sem=fwd_rs.at[way, c],
                device_id=(s, slot),
                device_id_type=MESH,
            ).wait_recv()

        base = pl.multiple_of(c * ch, ch)
        span = pl.ds(base, ch)
        sub = 64

        def norm(i, carry):
            at = pl.multiple_of(i * sub, sub)
            inner = pl.ds(pl.multiple_of(base + at, sub), sub)
            total = jnp.zeros((sub, DH), F32)
            squares = jnp.zeros((sub, DH), F32)
            for j in range(TP):
                for l in range(width // DH):
                    x = xg[j, inner, l * DH : (l + 1) * DH].astype(F32)
                    total = total + x
                    squares = squares + x * x
            mean = jnp.sum(total, axis=1, keepdims=True) / (TP * width)
            var = jnp.sum(squares, axis=1, keepdims=True) / (TP * width) - mean * mean
            scale = lax.rsqrt(var + LN_EPS)
            mean = jnp.broadcast_to(mean, (sub, DH))
            scale = jnp.broadcast_to(scale, (sub, DH))
            for j in range(TP):
                for l in range(width // DH):
                    x = xg[j, inner, l * DH : (l + 1) * DH].astype(F32)
                    f = j * width + l * DH
                    nb[pl.ds(at, sub), f : f + DH] = (
                        (x - mean) * scale * gain[0:1, f : f + DH]
                    ).astype(BF16)
            return carry

        lax.fori_loop(0, ch // sub, norm, 0)
        normed = nb[...]
        gsc[...] = dot_t(gt[...], normed)
        k_all = dot(normed, wk[...]).astype(BF16)
        q_all = dot(normed, wq[...]).astype(BF16)
        v_all = dot(normed, wv[...]).astype(BF16).astype(F32).T.astype(BF16)
        ks[span] = k_all
        qs[span] = q_all
        og[span] = dot(normed, wo[...]).astype(BF16)
        pool[pl.ds(pl.multiple_of(base + MARGIN, MARGIN), ch)] = dot(normed, wp[...]).astype(BF16)
        for h in range(2):
            vt[h, 0:DH, span] = v_all[h * DH : (h + 1) * DH]

        ins = []
        fgs = []
        for r in range(2):
            for h in range(2):
                ins.append(gsc[pl.ds(8 * r + 2 * t + h, 1), :])
                x = gsc[pl.ds(16 + 8 * r + 2 * t + h, 1), :] + bias[r, 2 * t + h]
                fgs.append(
                    (jnp.minimum(x, 0.0) - jnp.log1p(jnp.exp(-jnp.abs(x)))) * fscale[r : r + 1, span]
                    + fextra[r : r + 1, span]
                )
        blank = jnp.zeros((4, ch), F32)
        log_in = jnp.concatenate(ins + [blank], axis=0)
        log_fg = jnp.concatenate(fgs + [blank], axis=0)
        high = log_fg.astype(BF16).astype(F32)
        rest = log_fg - high
        mid = rest.astype(BF16).astype(F32)
        low = rest - mid
        parts = jnp.concatenate([high, mid, low, jnp.zeros((8, ch), F32)], axis=0).astype(BF16)
        sums = dot(parts, tri[...])
        sums = sums[0:8] + sums[8:16] + sums[16:24]
        which = lax.broadcasted_iota(jnp.int32, (8, ch), 0)
        falls = jnp.where(which < 2, sums[:, 0:ch], sums[:, ch : 2 * ch])
        a_row = log_in - falls
        a_col = jnp.concatenate([a_row, jnp.zeros((DH - 8, ch), F32)], axis=0).T
        peak = jnp.max(a_row, axis=1, keepdims=True)
        weight = jnp.exp(a_row - peak + half_log)
        ends = jnp.where(which[:, 0:1] < 2, falls[:, ch - 1 : ch], falls[:, 0:1])
        bs[c] = jnp.broadcast_to(ends, (8, DH))
        ms[c] = jnp.broadcast_to(ends + peak, (8, DH))
        rr = lax.broadcasted_iota(jnp.int32, (ch, ch), 0)
        cc = lax.broadcasted_iota(jnp.int32, (ch, ch), 1)
        for h in range(2):
            k_h = k_all[:, h * DH : (h + 1) * DH]
            q_h = q_all[:, h * DH : (h + 1) * DH]
            scores = dot_t(k_h, q_h)
            v_ext = vt[h, :, span]
            for r in range(2):
                ci = 2 * r + h
                inside = (rr <= cc) if r == 0 else (rr >= cc)
                expo = jnp.where(inside, a_col[:, ci : ci + 1], NEG_BIG)
                top = jnp.max(expo, axis=0, keepdims=True)
                probs = (scores * jnp.exp(expo - top + half_log)).astype(BF16)
                xl[ci, :, span] = dot(v_ext, probs)
                ar[pl.ds(ci, 1), span] = top
                cst[c, ci] = dot((v_ext.astype(F32) * weight[ci : ci + 1]).astype(BF16), k_h)
        return carry

    lax.fori_loop(0, TP, chunk, 0)

    to_prev = pltpu.make_async_remote_copy(
        src_ref=pool.at[pl.ds(MARGIN, RIM)],
        dst_ref=pool.at[pl.ds(MARGIN + rows, RIM)],
        send_sem=halo_ss.at[0],
        recv_sem=halo_rs.at[0],
        device_id=(lax.rem(s + ns - 1, ns), t),
        device_id_type=MESH,
    )
    to_next = pltpu.make_async_remote_copy(
        src_ref=pool.at[pl.ds(MARGIN + rows - RIM, RIM)],
        dst_ref=pool.at[pl.ds(MARGIN - RIM, RIM)],
        send_sem=halo_ss.at[1],
        recv_sem=halo_rs.at[1],
        device_id=(lax.rem(s + 1, ns), t),
        device_id_type=MESH,
    )

    for r in range(2):
        order = list(range(TP)) if r == 0 else list(range(TP - 1, -1, -1))
        for h in range(2):
            ci = 2 * r + h
            weights, fall, top = combine(
                [(bs[b, ci : ci + 1, :], ms[b, ci : ci + 1, :]) for b in order]
            )
            total = None
            for b, w in zip(order, weights):
                term = w * cst[b, ci]
                total = term if total is None else total + term
            sum_c[r, h] = total.astype(BF16)
            sum_s[r, h : h + 1, :] = fall
            sum_s[r, 2 + h : 3 + h, :] = top

    def pair(src_c, src_s, dst_c, dst_s, ss, rs, who):
        return [
            pltpu.make_async_remote_copy(
                src_ref=a, dst_ref=b, send_sem=ss.at[i], recv_sem=rs.at[i], device_id=who, device_id_type=MESH
            )
            for i, (a, b) in enumerate(((src_c, dst_c), (src_s, dst_s)))
        ]

    swap = pair(sum_c.at[1 - core], sum_s.at[1 - core], r0_c, r0_s, r0_ss, r0_rs, (partner, t))
    for one in swap:
        one.start()

    @pl.when(s > 0)
    def _():
        to_prev.start()

    @pl.when(s < ns - 1)
    def _():
        to_next.start()

    for one in swap:
        one.wait_recv()
    for h in range(2):
        weights, fall, top = combine(
            [
                (sum_s[core, h : h + 1, :], sum_s[core, 2 + h : 3 + h, :]),
                (r0_s[h : h + 1, :], r0_s[2 + h : 3 + h, :]),
            ]
        )
        y_c[yi, h] = (
            weights[0] * sum_c[core, h].astype(F32) + weights[1] * r0_c[h].astype(F32)
        ).astype(BF16)
        y_s[yi, h : h + 1, :] = fall
        y_s[yi, 2 + h : 3 + h, :] = top

    def y_pair(j, slot):
        who = ((zi * ny + lax.rem(yi + j, ny)) * 2 + core, t)
        return pair(
            y_c.at[slot], y_s.at[slot], y_c.at[slot], y_s.at[slot], y_ss.at[j], y_rs.at[slot], who
        )

    for j in range(1, ny):
        for one in y_pair(j, yi):
            one.start()

    @pl.when(s < ns - 1)
    def _():
        to_prev.wait_recv()

    @pl.when(s > 0)
    def _():
        to_next.wait_recv()

    half_span = jnp.left_shift(jnp.int32(1), t)
    map_own = gmap[t]
    scale_own = pscale[0:1, pl.ds(pl.multiple_of(t * DH, DH), DH)]

    def pool_copy(blk, off):
        return pltpu.make_async_remote_copy(
            src_ref=psend.at[blk],
            dst_ref=pbuf.at[t],
            send_sem=pool_ss.at[off],
            recv_sem=pool_rs.at[t],
            device_id=(s, blk),
            device_id_type=MESH,
        )

    ext = ch + 2 * MARGIN
    at_row = lax.broadcasted_iota(jnp.int32, (ch, ext), 0)
    at_col = lax.broadcasted_iota(jnp.int32, (ch, ext), 1) - MARGIN
    band = jnp.where((at_col >= at_row - half_span) & (at_col < at_row + half_span), 1.0, 0.0)
    band = band.astype(BF16)

    def pool_block(i, carry):
        off = jnp.where(i == 0, 2, jnp.where(i == 1, 1, jnp.where(i == 2, 3, 0)))
        blk = lax.rem(t + off, TP)
        base = pl.multiple_of(blk * ch, ch)
        near = pool[pl.ds(base, ext), :]
        pooled = dot(band, near)
        pos = s * rows + base + lax.broadcasted_iota(jnp.int32, (ch, 1), 0)
        counts = jnp.minimum(pos + half_span, ns * rows) - jnp.maximum(pos - half_span, 0)
        own = near[MARGIN : MARGIN + ch].astype(F32)
        contrast = (pooled / counts.astype(F32) - own).astype(BF16)
        result = (dot(contrast, map_own) * scale_own).astype(BF16)

        @pl.when(i < 3)
        def _():
            psend[blk] = result
            pool_copy(blk, off).start()

        @pl.when(i == 3)
        def _():
            pbuf[blk] = result

        return carry

    lax.fori_loop(0, TP, pool_block, 0)

    for j in range(1, ny):
        for one in y_pair(j, lax.rem(yi + j, ny)):
            one.wait_recv()
    y_slots = [core * (ny - 1) + i * step for i in range(ny)]
    for h in range(2):
        weights, fall, top = combine(
            [(y_s[i, h : h + 1, :], y_s[i, 2 + h : 3 + h, :]) for i in y_slots]
        )
        total = None
        for i, w in zip(y_slots, weights):
            term = w * y_c[i, h].astype(F32)
            total = term if total is None else total + term
        z_c[zi, h] = total.astype(BF16)
        z_s[zi, h : h + 1, :] = fall
        z_s[zi, 2 + h : 3 + h, :] = top

    def z_pair(j, slot):
        to = zi + j * step
        who = ((to * ny + yi) * 2 + core, t)
        return pair(
            z_c.at[slot], z_s.at[slot], z_c.at[slot], z_s.at[slot], z_ss.at[j], z_rs.at[slot], who
        )

    for j in range(1, nz):

        @pl.when((zi + j * step >= 0) & (zi + j * step < nz))
        def _():
            for one in z_pair(j, zi):
                one.start()

    for one in loads[5:7]:
        one.wait()
    for j in range(1, TP):
        src = lax.rem(t + j, TP)
        pltpu.make_async_remote_copy(
            src_ref=psend.at[src],
            dst_ref=pbuf.at[src],
            send_sem=pool_ss.at[j],
            recv_sem=pool_rs.at[src],
            device_id=(s, src),
            device_id_type=MESH,
        ).wait_recv()
    cols = 512

    def pool_out(i, carry):
        span = pl.ds(pl.multiple_of(i * cols, cols), cols)
        total = None
        for j in range(TP):
            term = dot(pbuf[j], wpo[j * DH : (j + 1) * DH, span])
            total = term if total is None else total + term
        acc[:, span] = total
        return carry

    lax.fori_loop(0, acc.shape[1] // cols, pool_out, 0)

    for j in range(1, nz):
        src = zi - j * step

        @pl.when((src >= 0) & (src < nz))
        def _():
            who = ((src * ny + yi) * 2 + core, t)
            for one in pair(
                z_c.at[src], z_s.at[src], z_c.at[src], z_s.at[src], z_ss.at[j], z_rs.at[src], who
            ):
                one.wait_recv()

    y_rel = jnp.where(core == 0, yi, ny - 1 - yi)
    z_rel = jnp.where(core == 0, zi, nz - 1 - zi)
    z_slots = [core * (nz - 1) + i * step for i in range(nz - 1)]
    for h in range(2):
        items = [(jnp.zeros((1, DH), F32), jnp.full((1, DH), start_m[core, h], F32))]
        for i, slot in enumerate(z_slots):
            valid = i < z_rel
            items.append(
                (
                    jnp.where(valid, z_s[slot, h : h + 1, :], 0.0),
                    jnp.where(valid, z_s[slot, 2 + h : 3 + h, :], NEG_BIG),
                )
            )
        for i, slot in enumerate(y_slots[: ny - 1]):
            valid = i < y_rel
            items.append(
                (
                    jnp.where(valid, y_s[slot, h : h + 1, :], 0.0),
                    jnp.where(valid, y_s[slot, 2 + h : 3 + h, :], NEG_BIG),
                )
            )
        weights, fall, top = combine(items)
        total = None
        for slot, w in zip(z_slots, weights[1 : 1 + len(z_slots)]):
            term = w * z_c[slot, h].astype(F32)
            total = term if total is None else total + term
        for slot, w in zip(y_slots[: ny - 1], weights[1 + len(z_slots) :]):
            term = w * y_c[slot, h].astype(F32)
            total = term if total is None else total + term
        ent_c[core, h] = total
        ent_c[core, h, 0:DH, :] += weights[0] * start_c[core, h]
        ent_c[core, h, DH : DH + 1, :] += weights[0] * start_n[core, h : h + 1, :]
        ent_m[core, h : h + 1, :] = top
        weights, fall, later = combine(
            [
                (jnp.zeros((1, DH), F32), top),
                (sum_s[core, h : h + 1, :], sum_s[core, 2 + h : 3 + h, :]),
            ]
        )
        p_c[h] = (weights[0] * ent_c[core, h] + weights[1] * sum_c[core, h].astype(F32)).astype(BF16)
        p_s[h : h + 1, :] = later
    give = pair(p_c, p_s, r3_c, r3_s, r3_ss, r3_rs, (partner, t))
    for one in give:
        one.start()
    for one in give:
        one.wait_recv()
    for h in range(2):
        ent_c[1 - core, h] = r3_c[h].astype(F32)
        ent_m[1 - core, h : h + 1, :] = r3_s[h : h + 1, :]

    for r in range(2):
        order = list(range(TP)) if r == 0 else list(range(TP - 1, -1, -1))
        for h in range(2):
            ci = 2 * r + h
            state = ent_c[r, h]
            top = ent_m[r, h : h + 1, :]
            for at, b in enumerate(order):
                est[b, ci] = state.astype(BF16)
                em[b, ci : ci + 1, :] = top
                if at < TP - 1:
                    weights, fall, later = combine(
                        [
                            (top, top),
                            (bs[b, ci : ci + 1, :], ms[b, ci : ci + 1, :]),
                        ]
                    )
                    state = weights[0] * state + weights[1] * cst[b, ci]
                    top = later

    def mem_copy(blk, off):
        return pltpu.make_async_remote_copy(
            src_ref=msend.at[blk],
            dst_ref=mbuf.at[t],
            send_sem=mem_ss.at[off],
            recv_sem=mem_rs.at[t],
            device_id=(s, blk),
            device_id_type=MESH,
        )

    def finish(i, carry):
        off = jnp.where(i == 0, 2, jnp.where(i == 1, 1, jnp.where(i == 2, 3, 0)))
        blk = lax.rem(t + off, TP)
        span = pl.ds(pl.multiple_of(blk * ch, ch), ch)
        pieces = []
        for h in range(2):
            q_h = qs[span, h * DH : (h + 1) * DH]
            hidden = None
            for r in range(2):
                ci = 2 * r + h
                from_state = dot_t(est[blk, ci], q_h)
                local_top = ar[pl.ds(ci, 1), span]
                state_top = em[blk, ci : ci + 1, 0:1]
                joint = jnp.maximum(local_top, state_top)
                local_w = jnp.exp(local_top - joint)
                state_w = jnp.exp(state_top - joint)
                den = (
                    local_w * xl[ci, DH : DH + 1, span] + state_w * from_state[DH : DH + 1]
                )
                inverse = 1.0 / jnp.maximum(jnp.abs(den), 1.0)
                term = (local_w * inverse) * xl[ci, 0:DH, span] + (state_w * inverse) * from_state[0:DH]
                hidden = term if hidden is None else hidden + term
            mean = jnp.mean(hidden, axis=0, keepdims=True)
            centred = hidden - mean
            var = jnp.mean(centred * centred, axis=0, keepdims=True)
            scaled = (centred * lax.rsqrt(var + HEAD_EPS)).T
            g_at = pl.multiple_of(t * 2 * DH + h * DH, DH)
            gate = jax.nn.sigmoid(og[span, h * DH : (h + 1) * DH].astype(F32))
            pieces.append((scaled * hgain[0:1, pl.ds(g_at, DH)] * gate).astype(BF16))

        @pl.when(i < 3)
        def _():
            for h in range(2):
                msend[blk, :, h * DH : (h + 1) * DH] = pieces[h]
            mem_copy(blk, off).start()

        @pl.when(i == 3)
        def _():
            for h in range(2):
                mbuf[blk, :, h * DH : (h + 1) * DH] = pieces[h]

        return carry

    lax.fori_loop(0, TP, finish, 0)

    def mem_part(src, last):
        def body(i, carry):
            span = pl.ds(pl.multiple_of(i * cols, cols), cols)
            at = pl.multiple_of(src * 2 * DH, 2 * DH)
            total = acc[:, span] + dot(mbuf[src], wmo[pl.ds(at, 2 * DH), span])
            if last:
                out[:, span] = total.astype(BF16)
            else:
                acc[:, span] = total
            return carry

        lax.fori_loop(0, acc.shape[1] // cols, body, 0)

    mem_part(t, False)
    for j in (1, 3, 2):
        src = lax.rem(t + j, TP)
        pltpu.make_async_remote_copy(
            src_ref=msend.at[src],
            dst_ref=mbuf.at[src],
            send_sem=mem_ss.at[j],
            recv_sem=mem_rs.at[src],
            device_id=(s, src),
            device_id_type=MESH,
        ).wait_recv()
        mem_part(src, j == 2)

    for c in range(TP):
        for way in (0, 1):
            own_copy(c, way).wait_send()
            fwd_copy(c, way).wait_send()
    for one in swap + give:
        one.wait_send()

    @pl.when(s > 0)
    def _():
        to_prev.wait_send()

    @pl.when(s < ns - 1)
    def _():
        to_next.wait_send()

    for j in range(1, ny):
        for one in y_pair(j, yi):
            one.wait_send()
    for j in range(1, nz):

        @pl.when((zi + j * step >= 0) & (zi + j * step < nz))
        def _():
            for one in z_pair(j, zi):
                one.wait_send()

    for j in range(1, TP):
        blk = lax.rem(t + j, TP)
        pool_copy(blk, j).wait_send()
        mem_copy(blk, j).wait_send()


def per_device(ny, nz, *args):
    (
        tokens,
        input_norm_gain,
        pooling_input_matrix,
        query_projection_matrix,
        key_projection_matrix,
        value_projection_matrix,
        output_gate_matrix,
        input_gate_matrix,
        forget_gate_matrix,
        forget_gate_bias,
        log_forget_scale,
        extra_log_forget,
        starting_memory,
        starting_normalizer,
        starting_log_scale,
        pooling_group_map,
        pooling_channel_scale,
        memory_head_gain,
        pooling_output_matrix,
        memory_output_matrix,
    ) = args
    rows, width = tokens.shape
    model = width * TP
    ch = rows // TP
    vmem = pl.BlockSpec(memory_space=pltpu.VMEM)
    smem = pl.BlockSpec(memory_space=pltpu.SMEM)
    hbm = pl.BlockSpec(memory_space=pl.ANY)
    dma = pltpu.SemaphoreType.DMA
    scratch = [
        pltpu.VMEM((TP, rows, width), BF16),
        pltpu.VMEM((model, DH), BF16),
        pltpu.VMEM((model, 2 * DH), BF16),
        pltpu.VMEM((model, 2 * DH), BF16),
        pltpu.VMEM((model, 2 * DH), BF16),
        pltpu.VMEM((model, 2 * DH), BF16),
        pltpu.VMEM(pooling_output_matrix.shape, BF16),
        pltpu.VMEM(memory_output_matrix.shape, BF16),
        pltpu.VMEM((ch, model), BF16),
        pltpu.VMEM((rows, 2 * DH), BF16),
        pltpu.VMEM((rows, 2 * DH), BF16),
        pltpu.VMEM((2, EXT, rows), BF16),
        pltpu.VMEM((rows, 2 * DH), BF16),
        pltpu.VMEM((rows + 2 * MARGIN, DH), BF16),
        pltpu.VMEM((32, model), BF16),
        pltpu.VMEM((32, ch), F32),
        pltpu.VMEM((ch, 2 * ch), BF16),
        pltpu.VMEM((4, EXT, rows), F32),
        pltpu.VMEM((8, rows), F32),
        pltpu.VMEM((TP, 4, EXT, DH), F32),
        pltpu.VMEM((TP, 8, DH), F32),
        pltpu.VMEM((TP, 8, DH), F32),
        pltpu.VMEM((2, 2, EXT, DH), BF16),
        pltpu.VMEM((2, 8, DH), F32),
        pltpu.VMEM((2, EXT, DH), BF16),
        pltpu.VMEM((8, DH), F32),
        pltpu.VMEM((ny, 2, EXT, DH), BF16),
        pltpu.VMEM((ny, 8, DH), F32),
        pltpu.VMEM((nz, 2, EXT, DH), BF16),
        pltpu.VMEM((nz, 8, DH), F32),
        pltpu.VMEM((2, EXT, DH), BF16),
        pltpu.VMEM((8, DH), F32),
        pltpu.VMEM((2, EXT, DH), BF16),
        pltpu.VMEM((8, DH), F32),
        pltpu.VMEM((2, 2, EXT, DH), F32),
        pltpu.VMEM((2, 8, DH), F32),
        pltpu.VMEM((TP, 4, EXT, DH), BF16),
        pltpu.VMEM((TP, 8, DH), F32),
        pltpu.VMEM((TP, ch, DH), BF16),
        pltpu.VMEM((TP, ch, DH), BF16),
        pltpu.VMEM((TP, ch, 2 * DH), BF16),
        pltpu.VMEM((TP, ch, 2 * DH), BF16),
        pltpu.VMEM((ch, model), F32),
        dma((8,)),
        dma((2, TP)),
        dma((2, TP)),
        dma((2, TP)),
        dma((2, TP)),
        dma((2,)),
        dma((2,)),
        dma((ny, 2)),
        dma((ny, 2)),
        dma((nz, 2)),
        dma((nz, 2)),
        dma((2,)),
        dma((2,)),
        dma((2,)),
        dma((2,)),
        dma((TP,)),
        dma((TP,)),
        dma((TP,)),
        dma((TP,)),
    ]
    return pl.pallas_call(
        functools.partial(kernel, ny, nz),
        out_shape=jax.ShapeDtypeStruct((ch, model), BF16),
        in_specs=[
            hbm,
            vmem,
            hbm,
            hbm,
            hbm,
            hbm,
            hbm,
            vmem,
            vmem,
            smem,
            vmem,
            vmem,
            vmem,
            vmem,
            smem,
            vmem,
            vmem,
            vmem,
            hbm,
            hbm,
        ],
        out_specs=vmem,
        scratch_shapes=scratch,
        compiler_params=pltpu.CompilerParams(
            collective_id=0, has_side_effects=True, vmem_limit_bytes=60 * 2**20
        ),
    )(
        tokens,
        input_norm_gain.reshape(1, model),
        pooling_input_matrix,
        query_projection_matrix,
        key_projection_matrix,
        value_projection_matrix,
        output_gate_matrix,
        input_gate_matrix.transpose(1, 2, 0),
        forget_gate_matrix.transpose(1, 2, 0),
        forget_gate_bias,
        log_forget_scale,
        extra_log_forget,
        starting_memory,
        starting_normalizer,
        starting_log_scale,
        pooling_group_map,
        pooling_channel_scale.reshape(1, -1),
        memory_head_gain.reshape(1, -1),
        pooling_output_matrix,
        memory_output_matrix,
    )


def solution(mesh):
    chips = mesh.shape["sp"] // 2
    ny = math.isqrt(chips) if math.isqrt(chips) ** 2 == chips else chips
    nz = chips // ny
    placed = (
        P("sp", "tp"),
        P(),
        P(None, "tp"),
        P(None, "tp"),
        P(None, "tp"),
        P(None, "tp"),
        P(None, "tp"),
        P(),
        P(),
        P(),
        P(None, "sp"),
        P(None, "sp"),
        P(None, "tp", None, None),
        P(None, "tp", None),
        P(None, "tp"),
        P(),
        P(),
        P(),
        P(),
        P(),
    )
    return jax.shard_map(
        functools.partial(per_device, ny, nz),
        mesh=mesh,
        in_specs=placed,
        out_specs=P(("sp", "tp"), None),
        check_vma=False,
    )
```

```python
import functools
import math

import jax
import jax.numpy as jnp
from jax import lax
from jax.experimental import pallas as pl
from jax.experimental.pallas import tpu as pltpu
from jax.sharding import PartitionSpec as P

DH = 128
EXT = 144
TP = 4
NCH = 8
MARGIN = 64
RIM = 16
NEG_BIG = -1e30
LN_EPS = 1e-05
HEAD_EPS = 1e-06
MESH = pl.DeviceIdType.MESH
F32 = jnp.float32
BF16 = jnp.bfloat16
TRANS_B = (((1,), (1,)), ((), ()))


def dot(a, b):
    return jnp.dot(a, b, preferred_element_type=F32)


def dot_t(a, b):
    return lax.dot_general(a, b, TRANS_B, preferred_element_type=F32)


def combine(items):
    after = None
    logs = []
    for fall, top in reversed(items):
        logs.append(top if after is None else top + after)
        after = fall if after is None else after + fall
    logs.reverse()
    joint = functools.reduce(jnp.maximum, logs)
    return [jnp.exp(one - joint) for one in logs], after, joint


def kernel(
    ny,
    nz,
    tok,
    gain,
    wp_hbm,
    wq_hbm,
    wk_hbm,
    wv_hbm,
    wo_hbm,
    gin,
    gfg,
    bias,
    fscale,
    fextra,
    start_c,
    start_n,
    start_m,
    gmap,
    pscale,
    hgain,
    wpo_hbm,
    wmo_hbm,
    out,
    xg,
    wp,
    wq,
    wk,
    wv,
    wo,
    wpo,
    wmo,
    nb,
    qs,
    ks,
    vt,
    og,
    pool,
    gt,
    gsc,
    ac,
    tri,
    xl,
    ar,
    cst,
    bs,
    ms,
    sum_c,
    sum_s,
    r0_c,
    r0_s,
    y_c,
    y_s,
    z_c,
    z_s,
    p_c,
    p_s,
    r3_c,
    r3_s,
    ent_c,
    ent_m,
    est,
    em,
    psend,
    pbuf,
    msend,
    mbuf,
    acc,
    load_sem,
    own_ss,
    own_rs,
    fwd_ss,
    fwd_rs,
    r0_ss,
    r0_rs,
    y_ss,
    y_rs,
    z_ss,
    z_rs,
    r3_ss,
    r3_rs,
    halo_ss,
    halo_rs,
    pool_ss,
    pool_rs,
    mem_ss,
    mem_rs,
):
    rows = tok.shape[0]
    width = tok.shape[1]
    ch = rows // TP
    cr = rows // NCH
    hf = cr // 2
    t = lax.axis_index("tp")
    s = lax.axis_index("sp")
    ns = 2 * ny * nz
    core = lax.rem(s, 2)
    yi = lax.rem(s // 2, ny)
    zi = s // (2 * ny)
    partner = s + 1 - 2 * core
    right = lax.rem(t + 1, TP)
    left = lax.rem(t + 3, TP)
    step = 1 - 2 * core
    half_log = F32(0) + (-0.5 * math.log(DH))

    loads = []
    for index, (src, dst) in enumerate(
        (
            (wq_hbm, wq),
            (wk_hbm, wk),
            (wv_hbm, wv),
            (wo_hbm, wo),
            (wp_hbm, wp),
            (wpo_hbm, wpo),
            (wmo_hbm, wmo),
            (tok, xg.at[t]),
        )
    ):
        loads.append(pltpu.make_async_copy(src, dst, load_sem.at[index]))
    loads[7].start()

    barrier = pltpu.get_barrier_semaphore()
    peers = [(s, lax.rem(t + j, TP)) for j in range(1, TP)]
    peers.append((partner, t))
    peers += [((zi * ny + lax.rem(yi + j, ny)) * 2 + core, t) for j in range(1, ny)]
    peers += [((lax.rem(zi + j, nz) * ny + yi) * 2 + core, t) for j in range(1, nz)]
    peers += [(lax.rem(s + 1, ns), t), (lax.rem(s + ns - 1, ns), t)]
    pool[0:MARGIN] = jnp.zeros((MARGIN, DH), BF16)
    pool[MARGIN + rows : 2 * MARGIN + rows] = jnp.zeros((MARGIN, DH), BF16)
    z_c[...] = jnp.zeros_like(z_c)
    z_s[...] = jnp.zeros_like(z_s)
    for peer in peers:
        pl.semaphore_signal(barrier, inc=1, device_id=peer, device_id_type=MESH)
    pl.semaphore_wait(barrier, len(peers))

    def own_copy(c, way):
        span = pl.ds(pl.multiple_of(c * cr, cr), cr)
        return pltpu.make_async_remote_copy(
            src_ref=tok.at[span],
            dst_ref=xg.at[t, span],
            send_sem=own_ss.at[way, c],
            recv_sem=own_rs.at[way, c],
            device_id=(s, right if way == 0 else left),
            device_id_type=MESH,
        )

    def fwd_copy(c, way):
        span = pl.ds(pl.multiple_of(c * cr + way * hf, hf), hf)
        slot = left if way == 0 else right
        return pltpu.make_async_remote_copy(
            src_ref=xg.at[slot, span],
            dst_ref=xg.at[slot, span],
            send_sem=fwd_ss.at[way, c],
            recv_sem=fwd_rs.at[way, c],
            device_id=(s, right if way == 0 else left),
            device_id_type=MESH,
        )

    for c in (0, 1):
        for way in (0, 1):
            own_copy(c, way).start()
    for one in loads[:7]:
        one.start()

    gt[...] = jnp.concatenate(
        [gin[0].astype(F32), gin[1].astype(F32), gfg[0].astype(F32), gfg[1].astype(F32)], axis=0
    ).astype(BF16)
    row_of = lax.broadcasted_iota(jnp.int32, (ch, ch), 0)
    col_of = lax.broadcasted_iota(jnp.int32, (ch, ch), 1)
    tri[:, 0:ch] = jnp.where(row_of <= col_of, 1.0, 0.0).astype(BF16)
    tri[:, ch : 2 * ch] = jnp.where(row_of >= col_of, 1.0, 0.0).astype(BF16)
    tail = lax.broadcasted_iota(jnp.int32, (EXT - DH, rows), 0)
    ones_row = jnp.where(tail == 0, 1.0, 0.0).astype(BF16)
    for h in range(2):
        vt[h, DH:EXT, :] = ones_row

    loads[7].wait()
    for way in (0, 1):
        own_copy(0, way).wait_recv()
        fwd_copy(0, way).start()
        own_copy(2, way).start()
    for one in loads[:5]:
        one.wait()

    def project_state(c):
        span = pl.ds(pl.multiple_of(c * cr, cr), cr)
        normed = nb[...]
        gsc[:, span] = dot_t(gt[...], normed)
        ks[span] = dot(normed, wk[...]).astype(BF16)
        v_all = dot(normed, wv[...]).astype(BF16).astype(F32).T.astype(BF16)
        for h in range(2):
            vt[h, 0:DH, span] = v_all[h * DH : (h + 1) * DH]

    def project_rest(c):
        base = pl.multiple_of(c * cr, cr)
        span = pl.ds(base, cr)
        normed = nb[...]
        qs[span] = dot(normed, wq[...]).astype(BF16)
        og[span] = dot(normed, wo[...]).astype(BF16)
        pool[pl.ds(pl.multiple_of(base + MARGIN, MARGIN), cr)] = dot(normed, wp[...]).astype(BF16)

    def state_part(b):
        span = pl.ds(pl.multiple_of(b * ch, ch), ch)
        ins = []
        fgs = []
        for r in range(2):
            for h in range(2):
                ins.append(gsc[pl.ds(8 * r + 2 * t + h, 1), span])
                x = gsc[pl.ds(16 + 8 * r + 2 * t + h, 1), span] + bias[r, 2 * t + h]
                fgs.append(
                    (jnp.minimum(x, 0.0) - jnp.log1p(jnp.exp(-jnp.abs(x)))) * fscale[r : r + 1, span]
                    + fextra[r : r + 1, span]
                )
        blank = jnp.zeros((4, ch), F32)
        log_in = jnp.concatenate(ins + [blank], axis=0)
        log_fg = jnp.concatenate(fgs + [blank], axis=0)
        high = log_fg.astype(BF16).astype(F32)
        rest = log_fg - high
        mid = rest.astype(BF16).astype(F32)
        low = rest - mid
        parts = jnp.concatenate([high, mid, low, jnp.zeros((8, ch), F32)], axis=0).astype(BF16)
        sums = dot(parts, tri[...])
        sums = sums[0:8] + sums[8:16] + sums[16:24]
        which = lax.broadcasted_iota(jnp.int32, (8, ch), 0)
        falls = jnp.where(which < 2, sums[:, 0:ch], sums[:, ch : 2 * ch])
        a_row = log_in - falls
        ac[span] = jnp.concatenate([a_row, jnp.zeros((DH - 8, ch), F32)], axis=0).T
        peak = jnp.max(a_row, axis=1, keepdims=True)
        weight = jnp.exp(a_row - peak + half_log)
        ends = jnp.where(which[:, 0:1] < 2, falls[:, ch - 1 : ch], falls[:, 0:1])
        bs[b] = jnp.broadcast_to(ends, (8, DH))
        ms[b] = jnp.broadcast_to(ends + peak, (8, DH))
        for h in range(2):
            k_h = ks[span, h * DH : (h + 1) * DH]
            v_ext = vt[h, :, span].astype(F32)
            for r in range(2):
                ci = 2 * r + h
                cst[b, ci] = dot((v_ext * weight[ci : ci + 1]).astype(BF16), k_h)

    def output_part(b):
        span = pl.ds(pl.multiple_of(b * ch, ch), ch)
        rr = lax.broadcasted_iota(jnp.int32, (ch, ch), 0)
        cc = lax.broadcasted_iota(jnp.int32, (ch, ch), 1)
        for h in range(2):
            k_h = ks[span, h * DH : (h + 1) * DH]
            q_h = qs[span, h * DH : (h + 1) * DH]
            scores = dot_t(k_h, q_h)
            v_ext = vt[h, :, span]
            for r in range(2):
                ci = 2 * r + h
                inside = (rr <= cc) if r == 0 else (rr >= cc)
                expo = jnp.where(inside, ac[span, ci : ci + 1], NEG_BIG)
                top = jnp.max(expo, axis=0, keepdims=True)
                probs = (scores * jnp.exp(expo - top + half_log)).astype(BF16)
                xl[ci, :, span] = dot(v_ext, probs)
                ar[pl.ds(ci, 1), span] = top

    def chunk(c, carry):
        @pl.when(c + 1 < NCH)
        def _():
            for way in (0, 1):
                own_copy(c + 1, way).wait_recv()
                fwd_copy(c + 1, way).start()

        @pl.when(c + 3 < NCH)
        def _():
            for way in (0, 1):
                own_copy(c + 3, way).start()

        for way in (0, 1):
            slot = left if way == 0 else right
            span = pl.ds(pl.multiple_of(c * cr + way * hf, hf), hf)
            far = lax.rem(t + 2, TP)
            pltpu.make_async_remote_copy(
                src_ref=xg.at[far, span],
                dst_ref=xg.at[far, span],
                send_sem=fwd_ss.at[way, c],
                recv_sem=fwd_rs.at[way, c],
                device_id=(s, slot),
                device_id_type=MESH,
            ).wait_recv()

        base = pl.multiple_of(c * cr, cr)
        sub = 64

        def norm(i, carry):
            at = pl.multiple_of(i * sub, sub)
            inner = pl.ds(pl.multiple_of(base + at, sub), sub)
            total = jnp.zeros((sub, DH), F32)
            squares = jnp.zeros((sub, DH), F32)
            for j in range(TP):
                for l in range(width // DH):
                    x = xg[j, inner, l * DH : (l + 1) * DH].astype(F32)
                    total = total + x
                    squares = squares + x * x
            mean = jnp.sum(total, axis=1, keepdims=True) / (TP * width)
            var = jnp.sum(squares, axis=1, keepdims=True) / (TP * width) - mean * mean
            scale = lax.rsqrt(var + LN_EPS)
            mean = jnp.broadcast_to(mean, (sub, DH))
            scale = jnp.broadcast_to(scale, (sub, DH))
            for j in range(TP):
                for l in range(width // DH):
                    x = xg[j, inner, l * DH : (l + 1) * DH].astype(F32)
                    f = j * width + l * DH
                    nb[pl.ds(at, sub), f : f + DH] = (
                        (x - mean) * scale * gain[0:1, f : f + DH]
                    ).astype(BF16)
            return carry

        lax.fori_loop(0, cr // sub, norm, 0)
        project_state(c)

        @pl.when(c + 1 < NCH)
        def _():
            project_rest(c)

        @pl.when(lax.rem(c, 2) == 1)
        def _():
            state_part(c // 2)

        @pl.when((lax.rem(c, 2) == 0) & (c > 0))
        def _():
            output_part(c // 2 - 1)

        return carry

    lax.fori_loop(0, NCH, chunk, 0)

    to_prev = pltpu.make_async_remote_copy(
        src_ref=pool.at[pl.ds(MARGIN, RIM)],
        dst_ref=pool.at[pl.ds(MARGIN + rows, RIM)],
        send_sem=halo_ss.at[0],
        recv_sem=halo_rs.at[0],
        device_id=(lax.rem(s + ns - 1, ns), t),
        device_id_type=MESH,
    )
    to_next = pltpu.make_async_remote_copy(
        src_ref=pool.at[pl.ds(MARGIN + rows - RIM, RIM)],
        dst_ref=pool.at[pl.ds(MARGIN - RIM, RIM)],
        send_sem=halo_ss.at[1],
        recv_sem=halo_rs.at[1],
        device_id=(lax.rem(s + 1, ns), t),
        device_id_type=MESH,
    )

    for r in range(2):
        order = list(range(TP)) if r == 0 else list(range(TP - 1, -1, -1))
        for h in range(2):
            ci = 2 * r + h
            weights, fall, top = combine(
                [(bs[b, ci : ci + 1, :], ms[b, ci : ci + 1, :]) for b in order]
            )
            total = None
            for b, w in zip(order, weights):
                term = w * cst[b, ci]
                total = term if total is None else total + term
            sum_c[r, h] = total.astype(BF16)
            sum_s[r, h : h + 1, :] = fall
            sum_s[r, 2 + h : 3 + h, :] = top

    def pair(src_c, src_s, dst_c, dst_s, ss, rs, who):
        return [
            pltpu.make_async_remote_copy(
                src_ref=a, dst_ref=b, send_sem=ss.at[i], recv_sem=rs.at[i], device_id=who, device_id_type=MESH
            )
            for i, (a, b) in enumerate(((src_c, dst_c), (src_s, dst_s)))
        ]

    swap = pair(sum_c.at[1 - core], sum_s.at[1 - core], r0_c, r0_s, r0_ss, r0_rs, (partner, t))
    for one in swap:
        one.start()
    project_rest(NCH - 1)

    @pl.when(s > 0)
    def _():
        to_prev.start()

    @pl.when(s < ns - 1)
    def _():
        to_next.start()

    for one in swap:
        one.wait_recv()
    for h in range(2):
        weights, fall, top = combine(
            [
                (sum_s[core, h : h + 1, :], sum_s[core, 2 + h : 3 + h, :]),
                (r0_s[h : h + 1, :], r0_s[2 + h : 3 + h, :]),
            ]
        )
        y_c[yi, h] = (
            weights[0] * sum_c[core, h].astype(F32) + weights[1] * r0_c[h].astype(F32)
        ).astype(BF16)
        y_s[yi, h : h + 1, :] = fall
        y_s[yi, 2 + h : 3 + h, :] = top

    def y_pair(j, slot):
        who = ((zi * ny + lax.rem(yi + j, ny)) * 2 + core, t)
        return pair(
            y_c.at[slot], y_s.at[slot], y_c.at[slot], y_s.at[slot], y_ss.at[j], y_rs.at[slot], who
        )

    for j in range(1, ny):
        for one in y_pair(j, yi):
            one.start()

    output_part(TP - 1)

    @pl.when(s < ns - 1)
    def _():
        to_prev.wait_recv()

    @pl.when(s > 0)
    def _():
        to_next.wait_recv()

    half_span = jnp.left_shift(jnp.int32(1), t)
    map_own = gmap[t]
    scale_own = pscale[0:1, pl.ds(pl.multiple_of(t * DH, DH), DH)]

    def pool_copy(blk, off):
        return pltpu.make_async_remote_copy(
            src_ref=psend.at[blk],
            dst_ref=pbuf.at[t],
            send_sem=pool_ss.at[off],
            recv_sem=pool_rs.at[t],
            device_id=(s, blk),
            device_id_type=MESH,
        )

    ext = ch + 2 * MARGIN
    at_row = lax.broadcasted_iota(jnp.int32, (ch, ext), 0)
    at_col = lax.broadcasted_iota(jnp.int32, (ch, ext), 1) - MARGIN
    band = jnp.where((at_col >= at_row - half_span) & (at_col < at_row + half_span), 1.0, 0.0)
    band = band.astype(BF16)

    def pool_block(i, carry):
        off = jnp.where(i == 0, 2, jnp.where(i == 1, 1, jnp.where(i == 2, 3, 0)))
        blk = lax.rem(t + off, TP)
        base = pl.multiple_of(blk * ch, ch)
        near = pool[pl.ds(base, ext), :]
        pooled = dot(band, near)
        pos = s * rows + base + lax.broadcasted_iota(jnp.int32, (ch, 1), 0)
        counts = jnp.minimum(pos + half_span, ns * rows) - jnp.maximum(pos - half_span, 0)
        own = near[MARGIN : MARGIN + ch].astype(F32)
        contrast = (pooled / counts.astype(F32) - own).astype(BF16)
        result = (dot(contrast, map_own) * scale_own).astype(BF16)

        @pl.when(i < 3)
        def _():
            psend[blk] = result
            pool_copy(blk, off).start()

        @pl.when(i == 3)
        def _():
            pbuf[blk] = result

        return carry

    lax.fori_loop(0, TP, pool_block, 0)

    for j in range(1, ny):
        for one in y_pair(j, lax.rem(yi + j, ny)):
            one.wait_recv()
    y_slots = [core * (ny - 1) + i * step for i in range(ny)]
    for h in range(2):
        weights, fall, top = combine(
            [(y_s[i, h : h + 1, :], y_s[i, 2 + h : 3 + h, :]) for i in y_slots]
        )
        total = None
        for i, w in zip(y_slots, weights):
            term = w * y_c[i, h].astype(F32)
            total = term if total is None else total + term
        z_c[zi, h] = total.astype(BF16)
        z_s[zi, h : h + 1, :] = fall
        z_s[zi, 2 + h : 3 + h, :] = top

    def z_pair(j, slot):
        to = zi + j * step
        who = ((to * ny + yi) * 2 + core, t)
        return pair(
            z_c.at[slot], z_s.at[slot], z_c.at[slot], z_s.at[slot], z_ss.at[j], z_rs.at[slot], who
        )

    for j in range(1, nz):

        @pl.when((zi + j * step >= 0) & (zi + j * step < nz))
        def _():
            for one in z_pair(j, zi):
                one.start()

    for one in loads[5:7]:
        one.wait()
    for j in range(1, TP):
        src = lax.rem(t + j, TP)
        pltpu.make_async_remote_copy(
            src_ref=psend.at[src],
            dst_ref=pbuf.at[src],
            send_sem=pool_ss.at[j],
            recv_sem=pool_rs.at[src],
            device_id=(s, src),
            device_id_type=MESH,
        ).wait_recv()
    cols = 512

    def pool_out(i, carry):
        span = pl.ds(pl.multiple_of(i * cols, cols), cols)
        total = None
        for j in range(TP):
            term = dot(pbuf[j], wpo[j * DH : (j + 1) * DH, span])
            total = term if total is None else total + term
        acc[:, span] = total
        return carry

    lax.fori_loop(0, acc.shape[1] // cols, pool_out, 0)

    for j in range(1, nz):
        src = zi - j * step

        @pl.when((src >= 0) & (src < nz))
        def _():
            who = ((src * ny + yi) * 2 + core, t)
            for one in pair(
                z_c.at[src], z_s.at[src], z_c.at[src], z_s.at[src], z_ss.at[j], z_rs.at[src], who
            ):
                one.wait_recv()

    y_rel = jnp.where(core == 0, yi, ny - 1 - yi)
    z_rel = jnp.where(core == 0, zi, nz - 1 - zi)
    z_slots = [core * (nz - 1) + i * step for i in range(nz - 1)]
    for h in range(2):
        items = [(jnp.zeros((1, DH), F32), jnp.full((1, DH), start_m[core, h], F32))]
        for i, slot in enumerate(z_slots):
            valid = i < z_rel
            items.append(
                (
                    jnp.where(valid, z_s[slot, h : h + 1, :], 0.0),
                    jnp.where(valid, z_s[slot, 2 + h : 3 + h, :], NEG_BIG),
                )
            )
        for i, slot in enumerate(y_slots[: ny - 1]):
            valid = i < y_rel
            items.append(
                (
                    jnp.where(valid, y_s[slot, h : h + 1, :], 0.0),
                    jnp.where(valid, y_s[slot, 2 + h : 3 + h, :], NEG_BIG),
                )
            )
        weights, fall, top = combine(items)
        total = None
        for slot, w in zip(z_slots, weights[1 : 1 + len(z_slots)]):
            term = w * z_c[slot, h].astype(F32)
            total = term if total is None else total + term
        for slot, w in zip(y_slots[: ny - 1], weights[1 + len(z_slots) :]):
            term = w * y_c[slot, h].astype(F32)
            total = term if total is None else total + term
        ent_c[core, h] = total
        ent_c[core, h, 0:DH, :] += weights[0] * start_c[core, h]
        ent_c[core, h, DH : DH + 1, :] += weights[0] * start_n[core, h : h + 1, :]
        ent_m[core, h : h + 1, :] = top
        weights, fall, later = combine(
            [
                (jnp.zeros((1, DH), F32), top),
                (sum_s[core, h : h + 1, :], sum_s[core, 2 + h : 3 + h, :]),
            ]
        )
        p_c[h] = (weights[0] * ent_c[core, h] + weights[1] * sum_c[core, h].astype(F32)).astype(BF16)
        p_s[h : h + 1, :] = later
    give = pair(p_c, p_s, r3_c, r3_s, r3_ss, r3_rs, (partner, t))
    for one in give:
        one.start()
    for one in give:
        one.wait_recv()
    for h in range(2):
        ent_c[1 - core, h] = r3_c[h].astype(F32)
        ent_m[1 - core, h : h + 1, :] = r3_s[h : h + 1, :]

    for r in range(2):
        order = list(range(TP)) if r == 0 else list(range(TP - 1, -1, -1))
        for h in range(2):
            ci = 2 * r + h
            state = ent_c[r, h]
            top = ent_m[r, h : h + 1, :]
            for at, b in enumerate(order):
                est[b, ci] = state.astype(BF16)
                em[b, ci : ci + 1, :] = top
                if at < TP - 1:
                    weights, fall, later = combine(
                        [
                            (top, top),
                            (bs[b, ci : ci + 1, :], ms[b, ci : ci + 1, :]),
                        ]
                    )
                    state = weights[0] * state + weights[1] * cst[b, ci]
                    top = later

    def mem_copy(blk, off):
        return pltpu.make_async_remote_copy(
            src_ref=msend.at[blk],
            dst_ref=mbuf.at[t],
            send_sem=mem_ss.at[off],
            recv_sem=mem_rs.at[t],
            device_id=(s, blk),
            device_id_type=MESH,
        )

    def finish(i, carry):
        off = jnp.where(i == 0, 2, jnp.where(i == 1, 1, jnp.where(i == 2, 3, 0)))
        blk = lax.rem(t + off, TP)
        span = pl.ds(pl.multiple_of(blk * ch, ch), ch)
        pieces = []
        for h in range(2):
            q_h = qs[span, h * DH : (h + 1) * DH]
            hidden = None
            for r in range(2):
                ci = 2 * r + h
                from_state = dot_t(est[blk, ci], q_h)
                local_top = ar[pl.ds(ci, 1), span]
                state_top = em[blk, ci : ci + 1, 0:1]
                joint = jnp.maximum(local_top, state_top)
                local_w = jnp.exp(local_top - joint)
                state_w = jnp.exp(state_top - joint)
                den = (
                    local_w * xl[ci, DH : DH + 1, span] + state_w * from_state[DH : DH + 1]
                )
                inverse = 1.0 / jnp.maximum(jnp.abs(den), 1.0)
                term = (local_w * inverse) * xl[ci, 0:DH, span] + (state_w * inverse) * from_state[0:DH]
                hidden = term if hidden is None else hidden + term
            mean = jnp.mean(hidden, axis=0, keepdims=True)
            centred = hidden - mean
            var = jnp.mean(centred * centred, axis=0, keepdims=True)
            scaled = (centred * lax.rsqrt(var + HEAD_EPS)).T
            g_at = pl.multiple_of(t * 2 * DH + h * DH, DH)
            gate = jax.nn.sigmoid(og[span, h * DH : (h + 1) * DH].astype(F32))
            pieces.append((scaled * hgain[0:1, pl.ds(g_at, DH)] * gate).astype(BF16))

        @pl.when(i < 3)
        def _():
            for h in range(2):
                msend[blk, :, h * DH : (h + 1) * DH] = pieces[h]
            mem_copy(blk, off).start()

        @pl.when(i == 3)
        def _():
            for h in range(2):
                mbuf[blk, :, h * DH : (h + 1) * DH] = pieces[h]

        return carry

    lax.fori_loop(0, TP, finish, 0)

    def mem_part(src, last):
        def body(i, carry):
            span = pl.ds(pl.multiple_of(i * cols, cols), cols)
            at = pl.multiple_of(src * 2 * DH, 2 * DH)
            total = acc[:, span] + dot(mbuf[src], wmo[pl.ds(at, 2 * DH), span])
            if last:
                out[:, span] = total.astype(BF16)
            else:
                acc[:, span] = total
            return carry

        lax.fori_loop(0, acc.shape[1] // cols, body, 0)

    mem_part(t, False)
    for j in (1, 3, 2):
        src = lax.rem(t + j, TP)
        pltpu.make_async_remote_copy(
            src_ref=msend.at[src],
            dst_ref=mbuf.at[src],
            send_sem=mem_ss.at[j],
            recv_sem=mem_rs.at[src],
            device_id=(s, src),
            device_id_type=MESH,
        ).wait_recv()
        mem_part(src, j == 2)

    for c in range(NCH):
        for way in (0, 1):
            own_copy(c, way).wait_send()
            fwd_copy(c, way).wait_send()
    for one in swap + give:
        one.wait_send()

    @pl.when(s > 0)
    def _():
        to_prev.wait_send()

    @pl.when(s < ns - 1)
    def _():
        to_next.wait_send()

    for j in range(1, ny):
        for one in y_pair(j, yi):
            one.wait_send()
    for j in range(1, nz):

        @pl.when((zi + j * step >= 0) & (zi + j * step < nz))
        def _():
            for one in z_pair(j, zi):
                one.wait_send()

    for j in range(1, TP):
        blk = lax.rem(t + j, TP)
        pool_copy(blk, j).wait_send()
        mem_copy(blk, j).wait_send()


def far(x):
    return pltpu.with_memory_space_constraint(x, pltpu.HBM)


def per_device(ny, nz, *args):
    (
        tokens,
        input_norm_gain,
        pooling_input_matrix,
        query_projection_matrix,
        key_projection_matrix,
        value_projection_matrix,
        output_gate_matrix,
        input_gate_matrix,
        forget_gate_matrix,
        forget_gate_bias,
        log_forget_scale,
        extra_log_forget,
        starting_memory,
        starting_normalizer,
        starting_log_scale,
        pooling_group_map,
        pooling_channel_scale,
        memory_head_gain,
        pooling_output_matrix,
        memory_output_matrix,
    ) = args
    rows, width = tokens.shape
    model = width * TP
    ch = rows // TP
    vmem = pl.BlockSpec(memory_space=pltpu.VMEM)
    smem = pl.BlockSpec(memory_space=pltpu.SMEM)
    hbm = pl.BlockSpec(memory_space=pltpu.HBM)
    dma = pltpu.SemaphoreType.DMA
    scratch = [
        pltpu.VMEM((TP, rows, width), BF16),
        pltpu.VMEM((model, DH), BF16),
        pltpu.VMEM((model, 2 * DH), BF16),
        pltpu.VMEM((model, 2 * DH), BF16),
        pltpu.VMEM((model, 2 * DH), BF16),
        pltpu.VMEM((model, 2 * DH), BF16),
        pltpu.VMEM(pooling_output_matrix.shape, BF16),
        pltpu.VMEM(memory_output_matrix.shape, BF16),
        pltpu.VMEM((rows // NCH, model), BF16),
        pltpu.VMEM((rows, 2 * DH), BF16),
        pltpu.VMEM((rows, 2 * DH), BF16),
        pltpu.VMEM((2, EXT, rows), BF16),
        pltpu.VMEM((rows, 2 * DH), BF16),
        pltpu.VMEM((rows + 2 * MARGIN, DH), BF16),
        pltpu.VMEM((32, model), BF16),
        pltpu.VMEM((32, rows), F32),
        pltpu.VMEM((rows, DH), F32),
        pltpu.VMEM((ch, 2 * ch), BF16),
        pltpu.VMEM((4, EXT, rows), F32),
        pltpu.VMEM((8, rows), F32),
        pltpu.VMEM((TP, 4, EXT, DH), F32),
        pltpu.VMEM((TP, 8, DH), F32),
        pltpu.VMEM((TP, 8, DH), F32),
        pltpu.VMEM((2, 2, EXT, DH), BF16),
        pltpu.VMEM((2, 8, DH), F32),
        pltpu.VMEM((2, EXT, DH), BF16),
        pltpu.VMEM((8, DH), F32),
        pltpu.VMEM((ny, 2, EXT, DH), BF16),
        pltpu.VMEM((ny, 8, DH), F32),
        pltpu.VMEM((nz, 2, EXT, DH), BF16),
        pltpu.VMEM((nz, 8, DH), F32),
        pltpu.VMEM((2, EXT, DH), BF16),
        pltpu.VMEM((8, DH), F32),
        pltpu.VMEM((2, EXT, DH), BF16),
        pltpu.VMEM((8, DH), F32),
        pltpu.VMEM((2, 2, EXT, DH), F32),
        pltpu.VMEM((2, 8, DH), F32),
        pltpu.VMEM((TP, 4, EXT, DH), BF16),
        pltpu.VMEM((TP, 8, DH), F32),
        pltpu.VMEM((TP, ch, DH), BF16),
        pltpu.VMEM((TP, ch, DH), BF16),
        pltpu.VMEM((TP, ch, 2 * DH), BF16),
        pltpu.VMEM((TP, ch, 2 * DH), BF16),
        pltpu.VMEM((ch, model), F32),
        dma((8,)),
        dma((2, NCH)),
        dma((2, NCH)),
        dma((2, NCH)),
        dma((2, NCH)),
        dma((2,)),
        dma((2,)),
        dma((ny, 2)),
        dma((ny, 2)),
        dma((nz, 2)),
        dma((nz, 2)),
        dma((2,)),
        dma((2,)),
        dma((2,)),
        dma((2,)),
        dma((TP,)),
        dma((TP,)),
        dma((TP,)),
        dma((TP,)),
    ]
    return pl.pallas_call(
        functools.partial(kernel, ny, nz),
        out_shape=jax.ShapeDtypeStruct((ch, model), BF16),
        in_specs=[
            hbm,
            vmem,
            hbm,
            hbm,
            hbm,
            hbm,
            hbm,
            vmem,
            vmem,
            smem,
            vmem,
            vmem,
            vmem,
            vmem,
            smem,
            vmem,
            vmem,
            vmem,
            hbm,
            hbm,
        ],
        out_specs=vmem,
        scratch_shapes=scratch,
        compiler_params=pltpu.CompilerParams(
            collective_id=0, has_side_effects=True, vmem_limit_bytes=44 * 2**20
        ),
    )(
        far(tokens),
        far(input_norm_gain.reshape(1, model)),
        far(pooling_input_matrix),
        far(query_projection_matrix),
        far(key_projection_matrix),
        far(value_projection_matrix),
        far(output_gate_matrix),
        far(input_gate_matrix.transpose(1, 2, 0)),
        far(forget_gate_matrix.transpose(1, 2, 0)),
        far(forget_gate_bias),
        far(log_forget_scale),
        far(extra_log_forget),
        far(starting_memory),
        far(starting_normalizer),
        far(starting_log_scale),
        far(pooling_group_map),
        far(pooling_channel_scale.reshape(1, -1)),
        far(memory_head_gain.reshape(1, -1)),
        far(pooling_output_matrix),
        far(memory_output_matrix),
    )


def solution(mesh):
    chips = mesh.shape["sp"] // 2
    ny = math.isqrt(chips) if math.isqrt(chips) ** 2 == chips else chips
    nz = chips // ny
    placed = (
        P("sp", "tp"),
        P(),
        P(None, "tp"),
        P(None, "tp"),
        P(None, "tp"),
        P(None, "tp"),
        P(None, "tp"),
        P(),
        P(),
        P(),
        P(None, "sp"),
        P(None, "sp"),
        P(None, "tp", None, None),
        P(None, "tp", None),
        P(None, "tp"),
        P(),
        P(),
        P(),
        P(),
        P(),
    )
    return jax.shard_map(
        functools.partial(per_device, ny, nz),
        mesh=mesh,
        in_specs=placed,
        out_specs=P(("sp", "tp"), None),
        check_vma=False,
    )
```
